32 devices in a mesh: sp: 8 (over z, y), tp: 4 (over x, core).
Axes of the slice: x: 2, y: 2, z: 4, core: 2. Of those that a mesh axis runs over, the one named last changes fastest.
Arguments:
- layer_input: bfloat16 [6144, 2048], P('sp', 'tp'), may hold values from -6 to 6
- input_norm_gain: bfloat16 [2048], replicated, may hold values from 0.099609375 to 1.8984375
- query_weight: bfloat16 [2048, 2048], P(None, 'tp'), may hold values from -0.125 to 0.125
- forget_weight: bfloat16 [2048, 2048], P(None, 'tp'), may hold values from -0.125 to 0.125
- value_matrix: bfloat16 [2048, 2048], P(None, 'tp'), may hold values from -0.125 to 0.125
- output_gate_weight: bfloat16 [2048, 2048], P(None, 'tp'), may hold values from -0.125 to 0.125
- after_gate_weight: bfloat16 [2048, 2048], P(None, 'tp'), may hold values from -0.125 to 0.125
- before_gate_weight: bfloat16 [2048, 2048], P(None, 'tp'), may hold values from -0.125 to 0.125
- convolution_input_weight: bfloat16 [2048, 2048], P(None, 'tp'), may hold values from -0.125 to 0.125
- forget_minimum: float32 [2048], P('tp'), may hold values from 0.95 to 0.9999837
- surge_log_decay: float32 [6144, 2048], P('sp', 'tp'), may hold values from -2.2 to 0
- convolution_kernel: bfloat16 [3, 2048], P(None, 'tp'), may hold values from -4 to 4
- head_norm_gain: bfloat16 [128], replicated, may hold values from 0.099609375 to 1.8984375
- starting_state: float32 [16, 128, 128], P('tp', 'sp'), may hold values from -0.09375 to 0.09375
- recurrence_output_weight: bfloat16 [2048, 2048], P('tp'), may hold values from -0.09375 to 0.09375
- convolution_output_weight: bfloat16 [2048, 2048], P('tp'), may hold values from -0.09375 to 0.09375
- output_norm_gain: bfloat16 [2048], replicated, may hold values from 0.099609375 to 1.8984375
Outputs:
- layer_out: bfloat16 [6144, 2048], P(('sp', 'tp'))
The draws below stay inside these ranges and needn't reach their ends.
All inputs are finite; a program needn't handle non-finite values.
Results may differ from the reference program's by a relative error of at most 0.014.
Values may be sent and summed in bfloat16 or wider, within the bound.
A program may use at most 128 MiB of HBM per device.

```python
import jax
import jax.numpy as jnp
from jax import lax

D = 2048
HEADS = 16
DK = 128
DV = 128
CW = 2048
CK = 3
BLK = 64
TOKENS_PER_SHARD = 768
TOKENS = 6144
KEYW = 2048
VALW = 2048


def decay_tables(key):
    keys = jax.random.split(jax.random.fold_in(key, 11), 6)
    share = 0.5
    slow_head = jax.random.uniform(keys[0], (HEADS,), jnp.float32) < share
    slow = jnp.repeat(slow_head, DK)
    rate = jnp.exp(jax.random.uniform(keys[1], (HEADS * DK,), jnp.float32, jnp.log(0.1), jnp.log(0.6))) / TOKENS
    fast_floor = jax.random.uniform(keys[2], (HEADS * DK,), jnp.float32, 0.95, 0.99)
    forget_minimum = jnp.where(slow, 1.0 - rate, fast_floor)
    extra_decay = jnp.where(slow, rate, 0.03)
    decay_factor = jnp.exp(jax.random.uniform(keys[3], (TOKENS // TOKENS_PER_SHARD,), jnp.float32, jnp.log(0.5), jnp.log(2.0)))
    spots = jax.random.randint(keys[4], (3,), 0, TOKENS)
    losses = jnp.log(jax.random.uniform(keys[5], (3,), jnp.float32, 0.5, 0.8))
    position = jnp.arange(TOKENS)
    decay_surge = jnp.sum(jnp.where(position[:, None] == spots[None, :], losses[None, :], 0.0), axis=1)
    surge_log_decay = -jnp.repeat(decay_factor, TOKENS_PER_SHARD)[:, None] * extra_decay[None, :] + decay_surge[:, None]
    return (forget_minimum.astype(jnp.float32), surge_log_decay.astype(jnp.float32))


def draw_forget_minimum(key, part):
    return decay_tables(key)[0]


def draw_surge_log_decay(key, part):
    return decay_tables(key)[1]


def shard_levels(key, shape, pieces, least, largest):
    factor_of, own = 1.0, jax.random.fold_in(key, 6)
    for dim, blocks in pieces:
        draws = jnp.exp(jax.random.uniform(jax.random.fold_in(own, dim), (blocks,), jnp.float32, least / len(pieces), largest / len(pieces)))
        factor_of = factor_of * jnp.repeat(draws, shape[dim] // blocks).reshape([-1 if axis == dim else 1 for axis in range(len(shape))])
    return factor_of


def normal_values(key, dims, deviation, limit, cuts=(), held_as=jnp.bfloat16):
    entries = jax.random.normal(key, dims, jnp.float32) * deviation
    if len(cuts) > 0:
        entries = shard_levels(key, dims, cuts, -0.22, 0.18) * entries
    return jnp.clip(entries, min=-limit, max=limit).astype(held_as)


def setup_inputs(seed: int = 0) -> dict:
    key_list = jax.random.split(jax.random.key(seed), 18)
    return {
        "layer_input": normal_values(key_list[0], (TOKENS, D), 1.0, 6.0, ((0, 8), (1, 4))),
        "input_norm_gain": jnp.clip(1.0 + 0.18 * jax.random.normal(key_list[1], (D,), jnp.float32), 0.099609375, 1.8984375).astype(jnp.bfloat16),
        "query_weight": normal_values(key_list[2], (D, KEYW), D ** -0.5, 0.125, ((1, 4),)),
        "forget_weight": normal_values(key_list[3], (D, KEYW), D ** -0.5, 0.125, ((1, 4),)),
        "value_matrix": normal_values(key_list[4], (D, VALW), D ** -0.5, 0.125, ((1, 4),)),
        "output_gate_weight": normal_values(key_list[5], (D, VALW), D ** -0.5, 0.125, ((1, 4),)),
        "after_gate_weight": normal_values(key_list[6], (D, CW), D ** -0.5, 0.125, ((1, 4),)),
        "before_gate_weight": normal_values(key_list[7], (D, CW), D ** -0.5, 0.125, ((1, 4),)),
        "convolution_input_weight": normal_values(key_list[8], (D, CW), D ** -0.5, 0.125, ((1, 4),)),
        "forget_minimum": draw_forget_minimum(jax.random.fold_in(key_list[17], 71), 0),
        "surge_log_decay": draw_surge_log_decay(jax.random.fold_in(key_list[17], 71), 0),
        "convolution_kernel": normal_values(key_list[11], (CK, CW), 0.577, 4.0, ((1, 4),)),
        "head_norm_gain": jnp.clip(1.0 + 0.18 * jax.random.normal(key_list[12], (DV,), jnp.float32), 0.099609375, 1.8984375).astype(jnp.bfloat16),
        "starting_state": normal_values(key_list[13], (HEADS, DK, DV), (0.5 * TOKENS ** -0.5), 0.09375, ((0, 4), (1, 8)), jnp.float32),
        "recurrence_output_weight": normal_values(key_list[14], (VALW, D), (VALW + CW) ** -0.5, 0.09375, ((0, 4),)),
        "convolution_output_weight": normal_values(key_list[15], (CW, D), (VALW + CW) ** -0.5, 0.09375, ((0, 4),)),
        "output_norm_gain": jnp.clip(1.0 + 0.18 * jax.random.normal(key_list[16], (D,), jnp.float32), 0.099609375, 1.8984375).astype(jnp.bfloat16),
    }


EPS = 1e-06
PRECISE_PRODUCT = lax.Precision.HIGHEST

def rms_scale(value_rows):
    return lax.rsqrt(lax.optimization_barrier(jnp.mean(value_rows * value_rows, axis=-1, keepdims=True)) + EPS)

def project(normed, weight):
    return jnp.dot(normed, weight, preferred_element_type=jnp.float32).astype(jnp.bfloat16)

def block_pass(latent_state, inputs):
    query_rows, key_inputs, value_rows, forget_gate_logits = inputs
    cumulative_decay = jnp.cumsum(forget_gate_logits, axis=1)
    length = query_rows.shape[1]
    causal_masking = jnp.tril(jnp.ones((length, length), dtype=bool))[None, :, :, None]
    crossed_output = jnp.einsum('rmq,rqu->rmu', query_rows * jnp.exp(cumulative_decay), latent_state, precision=PRECISE_PRODUCT)
    decay = jnp.exp(jnp.where(causal_masking, cumulative_decay[:, :, None, :] - cumulative_decay[:, None, :, :], -jnp.inf))
    scores = jnp.einsum('htk,hsk,htsk->hts', query_rows, key_inputs, decay, precision=PRECISE_PRODUCT)
    o_intra = jnp.einsum('hts,hsv->htv', scores, value_rows, precision=PRECISE_PRODUCT)
    final_state = cumulative_decay[:, -1:, :]
    latent_state = jnp.exp(final_state[:, 0, :])[..., None] * latent_state + jnp.einsum('xar,xai->xri', key_inputs * jnp.exp(final_state - cumulative_decay), value_rows, precision=PRECISE_PRODUCT)
    return (latent_state, o_intra + crossed_output)

def reference(layer_input, input_norm_gain, query_weight, forget_weight, value_matrix, output_gate_weight, after_gate_weight, before_gate_weight, convolution_input_weight, forget_minimum, surge_log_decay, convolution_kernel, head_norm_gain, starting_state, recurrence_output_weight, convolution_output_weight, output_norm_gain):
    rows_f = layer_input.astype(jnp.float32)
    normed = (rows_f * rms_scale(rows_f) * input_norm_gain.astype(jnp.float32)).astype(jnp.bfloat16)
    query_raw = project(normed, query_weight)
    forget_raw = project(normed, forget_weight)
    value_raw = project(normed, value_matrix)
    outgate_raw = project(normed, output_gate_weight)
    postgate_raw = project(normed, after_gate_weight)
    pregate_raw = project(normed, before_gate_weight)
    convval_raw = project(normed, convolution_input_weight)
    forget_single = forget_raw.astype(jnp.float32)
    forget_gate_logits = jnp.logaddexp(jnp.log(forget_minimum), jnp.log1p(-forget_minimum) + jax.nn.log_sigmoid(forget_single)) + surge_log_decay
    key_inputs = (1.0 - forget_minimum) * jax.nn.sigmoid(-forget_single)
    query_rows = jax.nn.silu(query_raw.astype(jnp.float32)) * DK ** (-0.5)
    blocks = TOKENS // BLK

    def to_blocks(value_rows, width):
        return value_rows.reshape(blocks, BLK, HEADS, width).transpose(0, 2, 1, 3)
    _, outputs = lax.scan(block_pass, starting_state.astype(jnp.float32), (to_blocks(query_rows, DK), to_blocks(key_inputs, DK), to_blocks(value_raw.astype(jnp.float32), DV), to_blocks(forget_gate_logits, DK)))
    recurrence_step = outputs.transpose(0, 2, 1, 3).reshape(TOKENS, HEADS, DV)
    normed_heads = recurrence_step * rms_scale(recurrence_step) * head_norm_gain.astype(jnp.float32)
    rec_out = (normed_heads.reshape(TOKENS, HEADS * DV) * jax.nn.silu(outgate_raw.astype(jnp.float32))).astype(jnp.bfloat16)
    mixed_in = pregate_raw.astype(jnp.float32) * convval_raw.astype(jnp.float32)
    padded = jnp.concatenate([jnp.zeros((CK - 1, mixed_in.shape[1]), jnp.float32), mixed_in], axis=0)
    taps_f = convolution_kernel.astype(jnp.float32)
    conv_sum = padded[0:TOKENS] * taps_f[0]
    for offset in range(1, CK):
        conv_sum = conv_sum + padded[offset:offset + TOKENS] * taps_f[offset]
    conv_out = (postgate_raw.astype(jnp.float32) * conv_sum).astype(jnp.bfloat16)
    mixed = jnp.dot(rec_out, recurrence_output_weight, preferred_element_type=jnp.float32) + jnp.dot(conv_out, convolution_output_weight, preferred_element_type=jnp.float32)
    return (mixed * rms_scale(mixed) * output_norm_gain.astype(jnp.float32)).astype(jnp.bfloat16)
```

```python
import functools

import jax
import jax.numpy as jnp
from jax import lax
from jax.experimental import pallas as pl
from jax.experimental.pallas import tpu as pltpu
from jax.sharding import PartitionSpec as P

DK = 128
DV = 128
CK = 3
BLK = 64
ROWS = 128


EPS = 1e-06
F32 = jnp.float32
BF16 = jnp.bfloat16


def from_behind(value, axis, by):
    peers = lax.axis_size(axis)
    pairs = [(i, i + by) for i in range(peers) if 0 <= i + by < peers]
    return lax.ppermute(value, axis, pairs)


def rms_scale(value_rows):
    return lax.rsqrt(jnp.mean(value_rows * value_rows, axis=-1, keepdims=True) + EPS)


def nt_dot(a, b):
    return lax.dot_general(a, b, (((1,), (1,)), ((), ())), preferred_element_type=F32)


def tn_dot(a, b):
    return lax.dot_general(a, b, (((0,), (0,)), ((), ())), preferred_element_type=F32)


def local_kernel(
    heads, q_ref, f_ref, v_ref, surge_ref, fmin_ref, part_ref, shift_ref, state_ref, total_ref, st, run
):
    step = pl.program_id(0)

    @pl.when(step == 0)
    def _():
        st[...] = jnp.zeros_like(st)
        run[...] = jnp.zeros_like(run)

    row = lax.broadcasted_iota(jnp.int32, (BLK, BLK), 0)
    col = lax.broadcasted_iota(jnp.int32, (BLK, BLK), 1)
    causal = col <= row
    middle = (causal.astype(F32) - (col < BLK // 2).astype(F32))
    for b in range(q_ref.shape[0] // BLK):
        rows = slice(b * BLK, (b + 1) * BLK)
        forget = f_ref[rows, :].astype(F32)
        keys = (1.0 - fmin_ref[...]) * jax.nn.sigmoid(-forget)
        logs = jnp.log1p(-keys) + surge_ref[rows, :]
        rel = jnp.dot(middle, logs, precision=lax.Precision.HIGHEST, preferred_element_type=F32)
        mid = logs[0:1, :] - rel[0:1, :]
        tail = rel[BLK - 1 : BLK, :]
        raw = q_ref[rows, :].astype(F32)
        queries = raw * jax.nn.sigmoid(raw) * DK ** (-0.5)
        q_mid = queries * jnp.exp(rel)
        k_mid = keys * jnp.exp(-rel)
        q_in = q_mid * jnp.exp(mid)
        k_out = (k_mid * jnp.exp(tail)).astype(BF16)
        whole = jnp.exp(mid + tail)
        shift_ref[rows, :] = (q_in * jnp.exp(run[...])).astype(BF16)
        run[...] = run[...] + mid + tail
        q_mid = q_mid.astype(BF16)
        k_mid = k_mid.astype(BF16)
        q_in = q_in.astype(BF16)
        values = v_ref[rows, :]
        for h in range(heads):
            ch = slice(h * DK, (h + 1) * DK)
            scores = jnp.where(causal, nt_dot(q_mid[:, ch], k_mid[:, ch]), 0.0).astype(BF16)
            before = st[h]
            part_ref[rows, ch] = jnp.dot(
                scores, values[:, ch], preferred_element_type=F32
            ) + nt_dot(q_in[:, ch], before.astype(BF16))
            st[h] = before * whole[:, ch] + tn_dot(values[:, ch], k_out[:, ch])

    @pl.when(step == pl.num_programs(0) - 1)
    def _():
        for h in range(heads):
            state_ref[h] = st[h].T
        total_ref[...] = run[...]


def local_pass(query_raw, forget_raw, value_raw, surge, fmin):
    tokens, width = query_raw.shape
    heads = width // DK
    rows = ROWS if tokens % ROWS == 0 else BLK
    tile = pl.BlockSpec((rows, width), lambda i: (i, 0))
    line = pl.BlockSpec((1, width), lambda i: (0, 0))
    return pl.pallas_call(
        functools.partial(local_kernel, heads),
        grid=(tokens // rows,),
        in_specs=[tile, tile, tile, tile, line],
        out_specs=[
            tile,
            tile,
            pl.BlockSpec((heads, DK, DV), lambda i: (0, 0, 0)),
            line,
        ],
        out_shape=[
            jax.ShapeDtypeStruct((tokens, width), F32),
            jax.ShapeDtypeStruct((tokens, width), BF16),
            jax.ShapeDtypeStruct((heads, DK, DV), F32),
            jax.ShapeDtypeStruct((1, width), F32),
        ],
        scratch_shapes=[pltpu.VMEM((heads, DV, DK), F32), pltpu.VMEM((1, width), F32)],
        cost_estimate=pl.CostEstimate(
            flops=tokens * width * 1000, bytes_accessed=tokens * width * 16, transcendentals=0
        ),
        name="local_pass",
    )(query_raw, forget_raw, value_raw, surge, fmin)


def shards(
    layer_input,
    input_norm_gain,
    query_weight,
    forget_weight,
    value_matrix,
    output_gate_weight,
    after_gate_weight,
    before_gate_weight,
    convolution_input_weight,
    forget_minimum,
    surge_log_decay,
    convolution_kernel,
    head_norm_gain,
    starting_state,
    recurrence_output_weight,
    convolution_output_weight,
    output_norm_gain,
):
    tokens_dev = layer_input.shape[0]
    heads_local = query_weight.shape[1] // DK
    weight_list = (
        query_weight,
        forget_weight,
        value_matrix,
        output_gate_weight,
        after_gate_weight,
        before_gate_weight,
        convolution_input_weight,
    )
    collected_rows = lax.all_gather(layer_input, "tp", axis=1, tiled=True)
    rows_f = collected_rows.astype(jnp.float32)
    normed = (rows_f * rms_scale(rows_f) * input_norm_gain.astype(jnp.float32)).astype(jnp.bfloat16)
    projections = tuple(
        (
            jnp.dot(normed, weight, preferred_element_type=jnp.float32).astype(jnp.bfloat16)
            for weight in weight_list
        )
    )
    query_raw, forget_raw, value_raw, outgate_raw, postgate_raw, pregate_raw, convval_raw = (
        projections
    )
    partial_output, shifted_query, local_state, local_total = local_pass(
        query_raw, forget_raw, value_raw, surge_log_decay, forget_minimum[None, :]
    )
    local_total = local_total.reshape(heads_local, DK)
    moved_state, moved_total = (
        lax.all_to_all(local_state[None], "sp", split_axis=2, concat_axis=0, tiled=True),
        lax.all_to_all(
            local_total[None, :, :, None], "sp", split_axis=2, concat_axis=0, tiled=True
        ),
    )
    running = starting_state
    entering = []
    for i in range(moved_state.shape[0]):
        entering.append(running)
        running = jnp.exp(moved_total[i]) * running + moved_state[i]
    carried_state = lax.all_to_all(
        jnp.stack(entering), "sp", split_axis=0, concat_axis=2, tiled=True
    )[0].astype(BF16)
    recurrence_step = partial_output.reshape(tokens_dev, heads_local, DV) + jnp.einsum(
        "xoq,oqu->xou",
        shifted_query.reshape(tokens_dev, heads_local, DK),
        carried_state,
        preferred_element_type=F32,
    )
    normed_heads = recurrence_step * rms_scale(recurrence_step) * head_norm_gain.astype(jnp.float32)
    rec_out = (
        normed_heads.reshape(tokens_dev, heads_local * DV)
        * jax.nn.silu(outgate_raw.astype(jnp.float32))
    ).astype(jnp.bfloat16)
    mixed_in = pregate_raw.astype(jnp.float32) * convval_raw.astype(jnp.float32)
    rim_rows = from_behind(mixed_in[tokens_dev - (CK - 1) :], "sp", 1)
    padded = jnp.concatenate([rim_rows, mixed_in], axis=0)
    taps_f = convolution_kernel.astype(jnp.float32)
    conv_sum = padded[0:tokens_dev] * taps_f[0]
    for offset in range(1, CK):
        conv_sum = conv_sum + padded[offset : offset + tokens_dev] * taps_f[offset]
    conv_out = (postgate_raw.astype(jnp.float32) * conv_sum).astype(jnp.bfloat16)
    mixed = lax.psum_scatter(
        (
            jnp.dot(rec_out, recurrence_output_weight, preferred_element_type=jnp.float32)
            + jnp.dot(conv_out, convolution_output_weight, preferred_element_type=jnp.float32)
        ).astype(BF16),
        "tp",
        scatter_dimension=0,
        tiled=True,
    ).astype(F32)
    return (mixed * rms_scale(mixed) * output_norm_gain.astype(jnp.float32)).astype(jnp.bfloat16)


def solution(mesh):
    return jax.shard_map(
        shards,
        mesh=mesh,
        in_specs=(
            P("sp", "tp"),
            P(),
            P(None, "tp"),
            P(None, "tp"),
            P(None, "tp"),
            P(None, "tp"),
            P(None, "tp"),
            P(None, "tp"),
            P(None, "tp"),
            P("tp"),
            P("sp", "tp"),
            P(None, "tp"),
            P(),
            P("tp", "sp", None),
            P("tp", None),
            P("tp", None),
            P(),
        ),
        out_specs=P(("sp", "tp"), None),
        check_vma=False,
    )
```

```python
import functools

import jax
import jax.numpy as jnp
from jax import lax
from jax.experimental import pallas as pl
from jax.experimental.pallas import tpu as pltpu
from jax.sharding import PartitionSpec as P

DK = 128
DV = 128
CK = 3
BLK = 64
ROWS = 128


EPS = 1e-06
F32 = jnp.float32
BF16 = jnp.bfloat16
MESH = pl.DeviceIdType.MESH


def rms_scale(value_rows):
    return lax.rsqrt(jnp.mean(value_rows * value_rows, axis=-1, keepdims=True) + EPS)


def nt_dot(a, b):
    return lax.dot_general(a, b, (((1,), (1,)), ((), ())), preferred_element_type=F32)


def tn_dot(a, b):
    return lax.dot_general(a, b, (((0,), (0,)), ((), ())), preferred_element_type=F32)


def local_kernel(
    heads, q_ref, f_ref, v_ref, surge_ref, fmin_ref, part_ref, shift_ref, pack_ref, st, run
):
    step = pl.program_id(0)

    @pl.when(step == 0)
    def _():
        st[...] = jnp.zeros_like(st)
        run[...] = jnp.zeros_like(run)

    row = lax.broadcasted_iota(jnp.int32, (BLK, BLK), 0)
    col = lax.broadcasted_iota(jnp.int32, (BLK, BLK), 1)
    causal = col <= row
    middle = (causal.astype(F32) - (col < BLK // 2).astype(F32))
    for b in range(q_ref.shape[0] // BLK):
        rows = slice(b * BLK, (b + 1) * BLK)
        forget = f_ref[rows, :].astype(F32)
        keys = (1.0 - fmin_ref[...]) * jax.nn.sigmoid(-forget)
        logs = jnp.log1p(-keys) + surge_ref[rows, :]
        rel = jnp.dot(middle, logs, precision=lax.Precision.HIGHEST, preferred_element_type=F32)
        mid = logs[0:1, :] - rel[0:1, :]
        tail = rel[BLK - 1 : BLK, :]
        raw = q_ref[rows, :].astype(F32)
        queries = raw * jax.nn.sigmoid(raw) * DK ** (-0.5)
        q_mid = queries * jnp.exp(rel)
        k_mid = keys * jnp.exp(-rel)
        q_in = q_mid * jnp.exp(mid)
        k_out = (k_mid * jnp.exp(tail)).astype(BF16)
        whole = jnp.exp(mid + tail)
        shift_ref[rows, :] = (q_in * jnp.exp(run[...])).astype(BF16)
        run[...] = run[...] + mid + tail
        q_mid = q_mid.astype(BF16)
        k_mid = k_mid.astype(BF16)
        q_in = q_in.astype(BF16)
        values = v_ref[rows, :]
        for h in range(heads):
            ch = slice(h * DK, (h + 1) * DK)
            scores = jnp.where(causal, nt_dot(q_mid[:, ch], k_mid[:, ch]), 0.0).astype(BF16)
            before = st[h]
            part_ref[rows, ch] = jnp.dot(
                scores, values[:, ch], preferred_element_type=F32
            ) + nt_dot(q_in[:, ch], before.astype(BF16))
            st[h] = before * whole[:, ch] + tn_dot(values[:, ch], k_out[:, ch])

    @pl.when(step == pl.num_programs(0) - 1)
    def _():
        peers, _, piece, _ = pack_ref.shape
        lane = lax.broadcasted_iota(jnp.int32, (DK, DV), 1)
        whole = jnp.exp(run[...])
        decays = jnp.zeros((DK, DV), F32)
        for h in range(heads):
            ch = slice(h * DK, (h + 1) * DK)
            state = st[h].T
            decays = jnp.where(lane == h, jnp.broadcast_to(whole[:, ch], (DV, DK)).T, decays)
            for p in range(peers):
                pack_ref[p, h] = state[p * piece : (p + 1) * piece]
        for p in range(peers):
            pack_ref[p, heads] = decays[p * piece : (p + 1) * piece]


def local_pass(peers, query_raw, forget_raw, value_raw, surge, fmin):
    tokens, width = query_raw.shape
    heads = width // DK
    rows = ROWS if tokens % ROWS == 0 else BLK
    tile = pl.BlockSpec((rows, width), lambda i: (i, 0))
    line = pl.BlockSpec((1, width), lambda i: (0, 0))
    return pl.pallas_call(
        functools.partial(local_kernel, heads),
        grid=(tokens // rows,),
        in_specs=[tile, tile, tile, tile, line],
        out_specs=[
            tile,
            tile,
            pl.BlockSpec((peers, heads + 1, DK // peers, DV), lambda i: (0, 0, 0, 0)),
        ],
        out_shape=[
            jax.ShapeDtypeStruct((tokens, width), F32),
            jax.ShapeDtypeStruct((tokens, width), BF16),
            jax.ShapeDtypeStruct((peers, heads + 1, DK // peers, DV), F32),
        ],
        scratch_shapes=[pltpu.VMEM((heads, DV, DK), F32), pltpu.VMEM((1, width), F32)],
        cost_estimate=pl.CostEstimate(
            flops=tokens * width * 1000, bytes_accessed=tokens * width * 16, transcendentals=0
        ),
        name="local_pass",
    )(query_raw, forget_raw, value_raw, surge, fmin)


def tp_places():
    me = lax.axis_index("tp")
    pair, core = me // 2, me % 2
    partner = 2 * pair + (1 - core)
    cross = 2 * (1 - pair) + core
    far = 2 * (1 - pair) + (1 - core)
    return me, partner, cross, far


def aligned(start, size):
    return pl.ds(pl.multiple_of(start, size), size)


def project_kernel(count, chunk, x_ref, gain_ref, *refs):
    weights, outs = refs[:count], refs[count : 2 * count]
    wbuf, xg, nb, wsem, csend, crecv, psend, precv, fsend, frecv = refs[2 * count :]
    steps = x_ref.shape[0] // chunk
    width = x_ref.shape[1]
    peers = xg.shape[0]
    me, partner, cross, far = tp_places()
    for j in range(count):
        pltpu.make_async_copy(weights[j], wbuf.at[j], wsem.at[j]).start()
    barrier = pltpu.get_barrier_semaphore()
    for other in (partner, cross):
        pl.semaphore_signal(barrier, inc=1, device_id={"tp": other}, device_id_type=MESH)
    pl.semaphore_wait(barrier, 2)

    def hop(step, src, slot, to, send, recv):
        rows = aligned(step * chunk, chunk)
        return pltpu.make_async_remote_copy(
            src_ref=src.at[rows],
            dst_ref=xg.at[slot, rows],
            send_sem=send.at[step],
            recv_sem=recv.at[step],
            device_id={"tp": to},
            device_id_type=MESH,
        )

    for step in range(steps):
        hop(step, x_ref, me, cross, csend, crecv).start()
    for step in range(steps):
        hop(step, x_ref, me, partner, psend, precv).start()
    xg[me] = x_ref[...]

    @pl.loop(0, steps + 1)
    def _(step):
        @pl.when(step < steps)
        def _():
            hop(step, x_ref, cross, cross, csend, crecv).wait_recv()
            hop(step, xg.at[cross], cross, partner, fsend, frecv).start()

        @pl.when(step > 0)
        def _():
            now = step - 1
            hop(now, x_ref, partner, partner, psend, precv).wait_recv()
            hop(now, x_ref, far, partner, fsend, frecv).wait_recv()
            rows = aligned(now * chunk, chunk)
            total = jnp.zeros((chunk, 1), F32)
            for s in range(peers):
                piece = xg[s, rows].astype(F32)
                total = total + jnp.sum(piece * piece, axis=-1, keepdims=True)
            scale = lax.rsqrt(total / (peers * width) + EPS)
            for s in range(peers):
                cols = slice(s * width, (s + 1) * width)
                gain = gain_ref[:, cols].astype(F32)
                nb[:, cols] = (xg[s, rows].astype(F32) * scale * gain).astype(BF16)
            for j in range(count):

                @pl.when(now == 0)
                def _():
                    pltpu.make_async_copy(weights[j], wbuf.at[j], wsem.at[j]).wait()

                outs[j][rows, :] = jnp.dot(
                    nb[...], wbuf[j], preferred_element_type=F32
                ).astype(BF16)

    for step in range(steps):
        hop(step, x_ref, me, cross, csend, crecv).wait_send()
        hop(step, x_ref, me, partner, psend, precv).wait_send()
        hop(step, xg.at[cross], cross, partner, fsend, frecv).wait_send()


def project(peers, layer_input, gain, weights):
    tokens, width = layer_input.shape
    count, cols = len(weights), weights[0].shape[1]
    chunk = 256 if tokens % 256 == 0 else BLK
    steps = tokens // chunk
    vmem = pl.BlockSpec(memory_space=pltpu.VMEM)
    dma = pltpu.SemaphoreType.DMA((steps,))
    return pl.pallas_call(
        functools.partial(project_kernel, count, chunk),
        out_shape=[jax.ShapeDtypeStruct((tokens, cols), BF16)] * count,
        in_specs=[vmem, vmem] + [pl.BlockSpec(memory_space=pl.ANY)] * count,
        out_specs=[vmem] * count,
        scratch_shapes=[
            pltpu.VMEM((count,) + weights[0].shape, BF16),
            pltpu.VMEM((peers, tokens, width), BF16),
            pltpu.VMEM((chunk, peers * width), BF16),
            pltpu.SemaphoreType.DMA((count,)),
        ]
        + [dma] * 6,
        compiler_params=pltpu.CompilerParams(collective_id=0, has_side_effects=True),
        name="project",
    )(layer_input, gain, *weights)


def finish_kernel(
    heads,
    part_ref,
    shift_ref,
    pack_ref,
    start_ref,
    gate_ref,
    post_ref,
    pre_ref,
    conv_ref,
    taps_ref,
    hgain_ref,
    wr_ref,
    wc_ref,
    ogain_ref,
    out_ref,
    land,
    ent,
    back,
    halo,
    mix,
    conv,
    acc,
    pbuf,
    prcv,
    cbuf,
    crcv,
    land_state,
    s1,
    r1,
    s2,
    r2,
    hs,
    hr,
    ps,
    pr,
    cs,
    cr,
):
    tokens, width = part_ref.shape
    sp = lax.axis_size("sp")
    quarter = tokens // lax.axis_size("tp")
    half = quarter // 2
    me, partner, cross, far = tp_places()
    seq = lax.axis_index("sp")
    barrier = pltpu.get_barrier_semaphore()
    for other in (partner, cross):
        pl.semaphore_signal(barrier, inc=1, device_id={"tp": other}, device_id_type=MESH)
    for off in range(1, sp):
        pl.semaphore_signal(
            barrier, inc=1, device_id={"sp": (seq + off) % sp}, device_id_type=MESH
        )
    pl.semaphore_wait(barrier, 2 + sp - 1)

    def give(src, dst, send, recv, to):
        return pltpu.make_async_remote_copy(
            src_ref=src,
            dst_ref=dst,
            send_sem=send,
            recv_sem=recv,
            device_id=to,
            device_id_type=MESH,
        )

    def state_hop(src, dst, slot, to, send, recv):
        return give(src.at[to], dst.at[slot], send.at[to], recv.at[slot], {"sp": to})

    rim = halo.shape[1]

    def rim_hop(i, src):
        return give(
            src.at[pl.ds(tokens - rim, rim)], halo.at[i], hs.at[i], hr.at[i], {"sp": (seq + 1) % sp}
        )

    for off in range(1, sp):
        state_hop(pack_ref, land, seq, (seq + off) % sp, s1, r1).start()
    rim_hop(0, pre_ref).start()
    rim_hop(1, conv_ref).start()

    land[seq] = pack_ref[seq]
    pad = mix.shape[0] - tokens

    def fill(i):
        rows = aligned(i * quarter, quarter)
        mix[pl.ds(pl.multiple_of(pad + i * quarter, 8), quarter), :] = pre_ref[rows, :].astype(
            F32
        ) * conv_ref[rows, :].astype(F32)

    for i in range(tokens // quarter):
        fill(i)

    def convolve(i):
        rows = slice(i * quarter, (i + 1) * quarter)
        total = None
        for j in range(CK):
            first = pad + i * quarter + j - (CK - 1)
            term = mix[first : first + quarter, :] * taps_ref[j : j + 1, :].astype(F32)
            total = term if total is None else total + term
        conv[rows, :] = (post_ref[rows, :].astype(F32) * total).astype(BF16)

    for i in range(1, tokens // quarter):
        convolve(i)

    for off in range(1, sp):
        src = (seq + sp - off) % sp
        state_hop(pack_ref, land, src, (seq + off) % sp, s1, r1).wait_recv()
    running = [start_ref[h] for h in range(heads)]
    for i in range(sp):
        decays = land[i, heads]
        for h in range(heads):
            ent[i, h] = running[h]
            running[h] = decays[:, h : h + 1] * running[h] + land[i, h]
    back[seq] = ent[seq]
    for off in range(1, sp):
        state_hop(ent, back, seq, (seq + off) % sp, s2, r2).start()

    rim_hop(0, pre_ref).wait_recv()
    rim_hop(1, conv_ref).wait_recv()
    last = halo[0].astype(F32) * halo[1].astype(F32)
    mix[pad - 8 : pad, :] = jnp.where(seq > 0, last[rim - 8 :, :], 0.0)
    convolve(0)

    @pl.loop(0, tokens // quarter)
    def _(i):
        rows = aligned(i * quarter, quarter)
        acc[rows, :] = jnp.dot(conv[rows, :], wc_ref[...], preferred_element_type=F32)

    for off in range(1, sp):
        src = (seq + sp - off) % sp
        state_hop(ent, back, src, (seq + off) % sp, s2, r2).wait_recv()
    for h in range(heads):
        carried = jnp.concatenate([back[i, h] for i in range(sp)], axis=0).astype(BF16)
        land_state[h] = carried

    def mixed(which, s):
        rows = aligned(which * quarter + s * half, half)
        gated = []
        for h in range(heads):
            ch = slice(h * DV, (h + 1) * DV)
            recur = part_ref[rows, ch] + jnp.dot(
                shift_ref[rows, ch], land_state[h], preferred_element_type=F32
            )
            gate = gate_ref[rows, ch].astype(F32)
            gated.append(
                (
                    recur * rms_scale(recur) * hgain_ref[...].astype(F32) * (gate * jax.nn.sigmoid(gate))
                ).astype(BF16)
            )
        rec = jnp.concatenate(gated, axis=1)
        return acc[rows, :] + jnp.dot(rec, wr_ref[...], preferred_element_type=F32)

    def put(which, s):
        rows = aligned(which * quarter + s * half, half)
        acc[rows, :] = mixed(which, s)

    def partner_hop(i):
        return give(pbuf.at[i], prcv.at[i], ps.at[i], pr.at[i], {"tp": partner})

    def cross_hop(i):
        return give(cbuf.at[i], crcv.at[i], cs.at[i], cr.at[i], {"tp": cross})

    def share(which, s, slot):
        pbuf[slot] = mixed(which, s).astype(BF16)
        partner_hop(slot).start()

    def forward(s):
        rows = aligned(cross * quarter + s * half, half)
        partner_hop(s).wait_recv()
        cbuf[s] = (acc[rows, :] + prcv[s].astype(F32)).astype(BF16)
        cross_hop(s).start()

    share(far, 0, 0)
    put(cross, 0)
    share(far, 1, 1)
    forward(0)
    put(cross, 1)
    forward(1)
    share(partner, 0, 2)
    share(partner, 1, 3)
    put(me, 0)
    put(me, 1)
    for s in range(2):
        partner_hop(2 + s).wait_recv()
        cross_hop(s).wait_recv()
        rows = aligned(me * quarter + s * half, half)
        total = acc[rows, :] + prcv[2 + s].astype(F32) + crcv[s].astype(F32)
        out_ref[s * half : (s + 1) * half, :] = (
            total * rms_scale(total) * ogain_ref[...].astype(F32)
        ).astype(BF16)

    for off in range(1, sp):
        to = (seq + off) % sp
        state_hop(pack_ref, land, seq, to, s1, r1).wait_send()
        state_hop(ent, back, seq, to, s2, r2).wait_send()
    rim_hop(0, pre_ref).wait_send()
    rim_hop(1, conv_ref).wait_send()
    for i in range(4):
        partner_hop(i).wait_send()
    for i in range(2):
        cross_hop(i).wait_send()


def finish(sp, tp, part, shift, pack, start, gate, post, pre, convval, taps, hgain, wr, wc, ogain):
    tokens, width = part.shape
    heads = width // DV
    quarter, wide = tokens // tp, wr.shape[1]
    half = quarter // 2
    vmem = pl.BlockSpec(memory_space=pltpu.VMEM)
    pieces = (sp, heads, DK // sp, DV)
    dma = pltpu.SemaphoreType.DMA
    return pl.pallas_call(
        functools.partial(finish_kernel, heads),
        out_shape=jax.ShapeDtypeStruct((quarter, wide), BF16),
        in_specs=[vmem] * 13,
        out_specs=vmem,
        scratch_shapes=[
            pltpu.VMEM(pack.shape, F32),
            pltpu.VMEM(pieces, F32),
            pltpu.VMEM(pieces, F32),
            pltpu.VMEM((2, 16, width), BF16),
            pltpu.VMEM((tokens + 8, width), F32),
            pltpu.VMEM((tokens, width), BF16),
            pltpu.VMEM((tokens, wide), F32),
            pltpu.VMEM((4, half, wide), BF16),
            pltpu.VMEM((4, half, wide), BF16),
            pltpu.VMEM((2, half, wide), BF16),
            pltpu.VMEM((2, half, wide), BF16),
            pltpu.VMEM((heads, DK, DV), BF16),
        ]
        + [dma((sp,))] * 4
        + [dma((2,))] * 2
        + [dma((4,))] * 2
        + [dma((2,))] * 2,
        compiler_params=pltpu.CompilerParams(collective_id=1, has_side_effects=True),
        name="finish",
    )(part, shift, pack, start, gate, post, pre, convval, taps, hgain, wr, wc, ogain)


def shards(
    layer_input,
    input_norm_gain,
    query_weight,
    forget_weight,
    value_matrix,
    output_gate_weight,
    after_gate_weight,
    before_gate_weight,
    convolution_input_weight,
    forget_minimum,
    surge_log_decay,
    convolution_kernel,
    head_norm_gain,
    starting_state,
    recurrence_output_weight,
    convolution_output_weight,
    output_norm_gain,
):
    sp, tp = lax.axis_size("sp"), lax.axis_size("tp")
    weight_list = (
        query_weight,
        forget_weight,
        value_matrix,
        output_gate_weight,
        after_gate_weight,
        before_gate_weight,
        convolution_input_weight,
    )
    query_raw, forget_raw, value_raw, outgate_raw, postgate_raw, pregate_raw, convval_raw = project(
        tp, layer_input, input_norm_gain[None, :], weight_list
    )
    partial_output, shifted_query, state_pieces = local_pass(
        sp, query_raw, forget_raw, value_raw, surge_log_decay, forget_minimum[None, :]
    )
    return finish(
        sp,
        tp,
        partial_output,
        shifted_query,
        state_pieces,
        starting_state,
        outgate_raw,
        postgate_raw,
        pregate_raw,
        convval_raw,
        convolution_kernel,
        head_norm_gain[None, :],
        recurrence_output_weight,
        convolution_output_weight,
        output_norm_gain[None, :],
    )


def solution(mesh):
    return jax.shard_map(
        shards,
        mesh=mesh,
        in_specs=(
            P("sp", "tp"),
            P(),
            P(None, "tp"),
            P(None, "tp"),
            P(None, "tp"),
            P(None, "tp"),
            P(None, "tp"),
            P(None, "tp"),
            P(None, "tp"),
            P("tp"),
            P("sp", "tp"),
            P(None, "tp"),
            P(),
            P("tp", "sp", None),
            P("tp", None),
            P("tp", None),
            P(),
        ),
        out_specs=P(("sp", "tp"), None),
        check_vma=False,
    )
```

```python
import functools

import jax
import jax.numpy as jnp
from jax import lax
from jax.experimental import pallas as pl
from jax.experimental.pallas import tpu as pltpu
from jax.sharding import PartitionSpec as P

DK = 128
DV = 128
CK = 3
BLK = 64
ROWS = 256


EPS = 1e-06
F32 = jnp.float32
BF16 = jnp.bfloat16
MESH = pl.DeviceIdType.MESH


def rms_scale(value_rows):
    return lax.rsqrt(jnp.mean(value_rows * value_rows, axis=-1, keepdims=True) + EPS)


def nt_dot(a, b):
    return lax.dot_general(a, b, (((1,), (1,)), ((), ())), preferred_element_type=F32)


def tn_dot(a, b):
    return lax.dot_general(a, b, (((0,), (0,)), ((), ())), preferred_element_type=F32)


def local_kernel(
    heads, q_ref, f_ref, v_ref, surge_ref, fmin_ref, part_ref, shift_ref, pack_ref, decay_ref, st, run
):
    step = pl.program_id(0)

    @pl.when(step == 0)
    def _():
        st[...] = jnp.zeros_like(st)
        run[...] = jnp.zeros_like(run)

    row = lax.broadcasted_iota(jnp.int32, (BLK, BLK), 0)
    col = lax.broadcasted_iota(jnp.int32, (BLK, BLK), 1)
    causal = col <= row
    middle = (causal.astype(F32) - (col < BLK // 2).astype(F32)).astype(BF16)
    middle = jnp.concatenate([middle] * 3, axis=1)
    for b in range(q_ref.shape[0] // BLK):
        rows = slice(b * BLK, (b + 1) * BLK)
        forget = f_ref[rows, :].astype(F32)
        keys = (1.0 - fmin_ref[...]) * jax.nn.sigmoid(-forget)
        logs = jnp.log1p(-keys) + surge_ref[rows, :]
        high = logs.astype(BF16)
        rest = logs - high.astype(F32)
        next_term = rest.astype(BF16)
        low = (rest - next_term.astype(F32)).astype(BF16)
        terms = jnp.concatenate([high, next_term, low], axis=0)
        rel = jnp.dot(middle, terms, preferred_element_type=F32)
        mid = logs[0:1, :] - rel[0:1, :]
        tail = rel[BLK - 1 : BLK, :]
        raw = q_ref[rows, :].astype(F32)
        queries = raw * jax.nn.sigmoid(raw) * DK ** (-0.5)
        q_mid = queries * jnp.exp(rel)
        k_mid = keys * jnp.exp(-rel)
        q_in = q_mid * jnp.exp(mid)
        k_out = (k_mid * jnp.exp(tail)).astype(BF16)
        whole = jnp.exp(mid + tail)
        shift_ref[rows, :] = (q_in * jnp.exp(run[...])).astype(BF16)
        run[...] = run[...] + mid + tail
        q_mid = q_mid.astype(BF16)
        k_mid = k_mid.astype(BF16)
        q_in = q_in.astype(BF16)
        values = v_ref[rows, :]
        for h in range(heads):
            ch = slice(h * DK, (h + 1) * DK)
            scores = jnp.where(causal, nt_dot(q_mid[:, ch], k_mid[:, ch]), 0.0).astype(BF16)
            before = st[h]
            part_ref[rows, ch] = jnp.dot(
                scores, values[:, ch], preferred_element_type=F32
            ) + nt_dot(q_in[:, ch], before.astype(BF16))
            st[h] = before * whole[:, ch] + tn_dot(values[:, ch], k_out[:, ch])

    @pl.when(step == pl.num_programs(0) - 1)
    def _():
        peers, _, piece, _ = pack_ref.shape
        lane = lax.broadcasted_iota(jnp.int32, (DK, DV), 1)
        whole = jnp.exp(run[...])
        decays = jnp.zeros((DK, DV), F32)
        for h in range(heads):
            ch = slice(h * DK, (h + 1) * DK)
            state = st[h].T
            decays = jnp.where(lane == h, jnp.broadcast_to(whole[:, ch], (DV, DK)).T, decays)
            for p in range(peers):
                pack_ref[p, h] = state[p * piece : (p + 1) * piece].astype(BF16)
        for p in range(peers):
            decay_ref[p] = decays[p * piece : (p + 1) * piece]


def local_pass(peers, query_raw, forget_raw, value_raw, surge, fmin):
    tokens, width = query_raw.shape
    heads = width // DK
    rows = ROWS if tokens % ROWS == 0 else BLK
    tile = pl.BlockSpec((rows, width), lambda i: (i, 0))
    line = pl.BlockSpec((1, width), lambda i: (0, 0))
    return pl.pallas_call(
        functools.partial(local_kernel, heads),
        grid=(tokens // rows,),
        in_specs=[tile, tile, tile, tile, line],
        out_specs=[
            tile,
            tile,
            pl.BlockSpec((peers, heads, DK // peers, DV), lambda i: (0, 0, 0, 0)),
            pl.BlockSpec((peers, DK // peers, DV), lambda i: (0, 0, 0)),
        ],
        out_shape=[
            jax.ShapeDtypeStruct((tokens, width), F32),
            jax.ShapeDtypeStruct((tokens, width), BF16),
            jax.ShapeDtypeStruct((peers, heads, DK // peers, DV), BF16),
            jax.ShapeDtypeStruct((peers, DK // peers, DV), F32),
        ],
        scratch_shapes=[pltpu.VMEM((heads, DV, DK), F32), pltpu.VMEM((1, width), F32)],
        cost_estimate=pl.CostEstimate(
            flops=tokens * width * 1000, bytes_accessed=tokens * width * 16, transcendentals=0
        ),
        name="local_pass",
    )(query_raw, forget_raw, value_raw, surge, fmin)


def tp_places():
    me = lax.axis_index("tp")
    pair, core = me // 2, me % 2
    partner = 2 * pair + (1 - core)
    cross = 2 * (1 - pair) + core
    far = 2 * (1 - pair) + (1 - core)
    return me, partner, cross, far


def aligned(start, size):
    return pl.ds(pl.multiple_of(start, size), size)


def project_kernel(count, chunk, x_ref, gain_ref, *refs):
    weights, outs = refs[:count], refs[count : 2 * count]
    wbuf, xg, nb, wsem, csend, crecv, psend, precv, fsend, frecv = refs[2 * count :]
    steps = x_ref.shape[0] // chunk
    width = x_ref.shape[1]
    peers = xg.shape[0]
    me, partner, cross, far = tp_places()
    for j in range(count):
        pltpu.make_async_copy(weights[j], wbuf.at[j], wsem.at[j]).start()
    barrier = pltpu.get_barrier_semaphore()
    for other in (partner, cross):
        pl.semaphore_signal(barrier, inc=1, device_id={"tp": other}, device_id_type=MESH)
    pl.semaphore_wait(barrier, 2)

    def hop(step, src, slot, to, send, recv):
        rows = aligned(step * chunk, chunk)
        return pltpu.make_async_remote_copy(
            src_ref=src.at[rows],
            dst_ref=xg.at[slot, rows],
            send_sem=send.at[step],
            recv_sem=recv.at[step],
            device_id={"tp": to},
            device_id_type=MESH,
        )

    for step in range(steps):
        hop(step, x_ref, me, cross, csend, crecv).start()
    for step in range(steps):
        hop(step, x_ref, me, partner, psend, precv).start()
    xg[me] = x_ref[...]

    @pl.loop(0, steps + 1)
    def _(step):
        @pl.when(step < steps)
        def _():
            hop(step, x_ref, cross, cross, csend, crecv).wait_recv()
            hop(step, xg.at[cross], cross, partner, fsend, frecv).start()

        @pl.when(step > 0)
        def _():
            now = step - 1
            hop(now, x_ref, partner, partner, psend, precv).wait_recv()
            hop(now, x_ref, far, partner, fsend, frecv).wait_recv()
            rows = aligned(now * chunk, chunk)
            total = jnp.zeros((chunk, 1), F32)
            for s in range(peers):
                piece = xg[s, rows].astype(F32)
                total = total + jnp.sum(piece * piece, axis=-1, keepdims=True)
            scale = lax.rsqrt(total / (peers * width) + EPS)
            for s in range(peers):
                cols = slice(s * width, (s + 1) * width)
                gain = gain_ref[:, cols].astype(F32)
                nb[:, cols] = (xg[s, rows].astype(F32) * scale * gain).astype(BF16)
            for j in range(count):

                @pl.when(now == 0)
                def _():
                    pltpu.make_async_copy(weights[j], wbuf.at[j], wsem.at[j]).wait()

                outs[j][rows, :] = jnp.dot(
                    nb[...], wbuf[j], preferred_element_type=F32
                ).astype(BF16)

    for step in range(steps):
        hop(step, x_ref, me, cross, csend, crecv).wait_send()
        hop(step, x_ref, me, partner, psend, precv).wait_send()
        hop(step, xg.at[cross], cross, partner, fsend, frecv).wait_send()


def project(peers, layer_input, gain, weights):
    tokens, width = layer_input.shape
    count, cols = len(weights), weights[0].shape[1]
    chunk = 256 if tokens % 256 == 0 else BLK
    steps = tokens // chunk
    vmem = pl.BlockSpec(memory_space=pltpu.VMEM)
    dma = pltpu.SemaphoreType.DMA((steps,))
    return pl.pallas_call(
        functools.partial(project_kernel, count, chunk),
        out_shape=[jax.ShapeDtypeStruct((tokens, cols), BF16)] * count,
        in_specs=[vmem, vmem] + [pl.BlockSpec(memory_space=pl.ANY)] * count,
        out_specs=[vmem] * count,
        scratch_shapes=[
            pltpu.VMEM((count,) + weights[0].shape, BF16),
            pltpu.VMEM((peers, tokens, width), BF16),
            pltpu.VMEM((chunk, peers * width), BF16),
            pltpu.SemaphoreType.DMA((count,)),
        ]
        + [dma] * 6,
        compiler_params=pltpu.CompilerParams(collective_id=0, has_side_effects=True),
        name="project",
    )(layer_input, gain, *weights)


def finish_kernel(
    heads,
    part_ref,
    shift_ref,
    pack_ref,
    decay_ref,
    start_ref,
    gate_ref,
    post_ref,
    pre_ref,
    conv_ref,
    taps_ref,
    hgain_ref,
    wr_ref,
    wc_ref,
    ogain_ref,
    out_ref,
    land,
    land_decay,
    ent,
    back,
    halo,
    mix,
    conv,
    acc,
    pbuf,
    prcv,
    cbuf,
    crcv,
    land_state,
    s1,
    r1,
    sd,
    rd,
    s2,
    r2,
    hs,
    hr,
    ps,
    pr,
    cs,
    cr,
):
    tokens, width = part_ref.shape
    sp = lax.axis_size("sp")
    quarter = tokens // lax.axis_size("tp")
    half = quarter // 2
    me, partner, cross, far = tp_places()
    seq = lax.axis_index("sp")
    barrier = pltpu.get_barrier_semaphore()
    for other in (partner, cross):
        pl.semaphore_signal(barrier, inc=1, device_id={"tp": other}, device_id_type=MESH)
    for off in range(1, sp):
        pl.semaphore_signal(
            barrier, inc=1, device_id={"sp": (seq + off) % sp}, device_id_type=MESH
        )
    pl.semaphore_wait(barrier, 2 + sp - 1)

    def give(src, dst, send, recv, to):
        return pltpu.make_async_remote_copy(
            src_ref=src,
            dst_ref=dst,
            send_sem=send,
            recv_sem=recv,
            device_id=to,
            device_id_type=MESH,
        )

    def state_hop(src, dst, slot, to, send, recv):
        return give(src.at[to], dst.at[slot], send.at[to], recv.at[slot], {"sp": to})

    rim = halo.shape[1]

    def rim_hop(i, src):
        return give(
            src.at[pl.ds(tokens - rim, rim)], halo.at[i], hs.at[i], hr.at[i], {"sp": (seq + 1) % sp}
        )

    for off in range(1, sp):
        state_hop(decay_ref, land_decay, seq, (seq + off) % sp, sd, rd).start()
        state_hop(pack_ref, land, seq, (seq + off) % sp, s1, r1).start()
    rim_hop(0, pre_ref).start()
    rim_hop(1, conv_ref).start()

    land[seq] = pack_ref[seq]
    land_decay[seq] = decay_ref[seq]
    pad = mix.shape[0] - tokens

    def fill(i):
        rows = aligned(i * quarter, quarter)
        mix[pl.ds(pl.multiple_of(pad + i * quarter, 8), quarter), :] = pre_ref[rows, :].astype(
            F32
        ) * conv_ref[rows, :].astype(F32)

    for i in range(tokens // quarter):
        fill(i)

    def convolve(i):
        rows = slice(i * quarter, (i + 1) * quarter)
        total = None
        for j in range(CK):
            first = pad + i * quarter + j - (CK - 1)
            term = mix[first : first + quarter, :] * taps_ref[j : j + 1, :].astype(F32)
            total = term if total is None else total + term
        conv[rows, :] = (post_ref[rows, :].astype(F32) * total).astype(BF16)

    for i in range(1, tokens // quarter):
        convolve(i)

    for off in range(1, sp):
        src = (seq + sp - off) % sp
        state_hop(decay_ref, land_decay, src, (seq + off) % sp, sd, rd).wait_recv()
        state_hop(pack_ref, land, src, (seq + off) % sp, s1, r1).wait_recv()
    running = [start_ref[h] for h in range(heads)]
    for i in range(sp):
        decays = land_decay[i]
        for h in range(heads):
            ent[i, h] = running[h].astype(BF16)
            running[h] = decays[:, h : h + 1] * running[h] + land[i, h].astype(F32)
    back[seq] = ent[seq]
    for off in range(1, sp):
        state_hop(ent, back, seq, (seq + off) % sp, s2, r2).start()

    rim_hop(0, pre_ref).wait_recv()
    rim_hop(1, conv_ref).wait_recv()
    last = halo[0].astype(F32) * halo[1].astype(F32)
    mix[pad - 8 : pad, :] = jnp.where(seq > 0, last[rim - 8 :, :], 0.0)
    convolve(0)

    @pl.loop(0, tokens // quarter)
    def _(i):
        rows = aligned(i * quarter, quarter)
        acc[rows, :] = jnp.dot(conv[rows, :], wc_ref[...], preferred_element_type=F32)

    for off in range(1, sp):
        src = (seq + sp - off) % sp
        state_hop(ent, back, src, (seq + off) % sp, s2, r2).wait_recv()
    for h in range(heads):
        carried = jnp.concatenate([back[i, h].astype(F32) for i in range(sp)], axis=0).astype(BF16)
        land_state[h] = carried

    def mixed(which, s):
        rows = aligned(which * quarter + s * half, half)
        gated = []
        for h in range(heads):
            ch = slice(h * DV, (h + 1) * DV)
            recur = part_ref[rows, ch] + jnp.dot(
                shift_ref[rows, ch], land_state[h], preferred_element_type=F32
            )
            gate = gate_ref[rows, ch].astype(F32)
            gated.append(
                (
                    recur * rms_scale(recur) * hgain_ref[...].astype(F32) * (gate * jax.nn.sigmoid(gate))
                ).astype(BF16)
            )
        rec = jnp.concatenate(gated, axis=1)
        return acc[rows, :] + jnp.dot(rec, wr_ref[...], preferred_element_type=F32)

    def put(which, s):
        rows = aligned(which * quarter + s * half, half)
        acc[rows, :] = mixed(which, s)

    def partner_hop(i):
        return give(pbuf.at[i], prcv.at[i], ps.at[i], pr.at[i], {"tp": partner})

    def cross_hop(i):
        return give(cbuf.at[i], crcv.at[i], cs.at[i], cr.at[i], {"tp": cross})

    def share(which, s, slot):
        pbuf[slot] = mixed(which, s).astype(BF16)
        partner_hop(slot).start()

    def forward(s):
        rows = aligned(cross * quarter + s * half, half)
        partner_hop(s).wait_recv()
        cbuf[s] = (acc[rows, :] + prcv[s].astype(F32)).astype(BF16)
        cross_hop(s).start()

    share(far, 0, 0)
    put(cross, 0)
    share(far, 1, 1)
    forward(0)
    put(cross, 1)
    forward(1)
    share(partner, 0, 2)
    share(partner, 1, 3)
    put(me, 0)
    put(me, 1)
    for s in range(2):
        partner_hop(2 + s).wait_recv()
        cross_hop(s).wait_recv()
        rows = aligned(me * quarter + s * half, half)
        total = acc[rows, :] + prcv[2 + s].astype(F32) + crcv[s].astype(F32)
        out_ref[s * half : (s + 1) * half, :] = (
            total * rms_scale(total) * ogain_ref[...].astype(F32)
        ).astype(BF16)

    for off in range(1, sp):
        to = (seq + off) % sp
        state_hop(decay_ref, land_decay, seq, to, sd, rd).wait_send()
        state_hop(pack_ref, land, seq, to, s1, r1).wait_send()
        state_hop(ent, back, seq, to, s2, r2).wait_send()
    rim_hop(0, pre_ref).wait_send()
    rim_hop(1, conv_ref).wait_send()
    for i in range(4):
        partner_hop(i).wait_send()
    for i in range(2):
        cross_hop(i).wait_send()


def finish(sp, tp, part, shift, pack, decay, start, gate, post, pre, convval, taps, hgain, wr, wc, ogain):
    tokens, width = part.shape
    heads = width // DV
    quarter, wide = tokens // tp, wr.shape[1]
    half = quarter // 2
    vmem = pl.BlockSpec(memory_space=pltpu.VMEM)
    pieces = (sp, heads, DK // sp, DV)
    dma = pltpu.SemaphoreType.DMA
    return pl.pallas_call(
        functools.partial(finish_kernel, heads),
        out_shape=jax.ShapeDtypeStruct((quarter, wide), BF16),
        in_specs=[vmem] * 14,
        out_specs=vmem,
        scratch_shapes=[
            pltpu.VMEM(pieces, BF16),
            pltpu.VMEM(decay.shape, F32),
            pltpu.VMEM(pieces, BF16),
            pltpu.VMEM(pieces, BF16),
            pltpu.VMEM((2, 16, width), BF16),
            pltpu.VMEM((tokens + 8, width), F32),
            pltpu.VMEM((tokens, width), BF16),
            pltpu.VMEM((tokens, wide), F32),
            pltpu.VMEM((4, half, wide), BF16),
            pltpu.VMEM((4, half, wide), BF16),
            pltpu.VMEM((2, half, wide), BF16),
            pltpu.VMEM((2, half, wide), BF16),
            pltpu.VMEM((heads, DK, DV), BF16),
        ]
        + [dma((sp,))] * 6
        + [dma((2,))] * 2
        + [dma((4,))] * 2
        + [dma((2,))] * 2,
        compiler_params=pltpu.CompilerParams(collective_id=1, has_side_effects=True),
        name="finish",
    )(part, shift, pack, decay, start, gate, post, pre, convval, taps, hgain, wr, wc, ogain)


def shards(
    layer_input,
    input_norm_gain,
    query_weight,
    forget_weight,
    value_matrix,
    output_gate_weight,
    after_gate_weight,
    before_gate_weight,
    convolution_input_weight,
    forget_minimum,
    surge_log_decay,
    convolution_kernel,
    head_norm_gain,
    starting_state,
    recurrence_output_weight,
    convolution_output_weight,
    output_norm_gain,
):
    sp, tp = lax.axis_size("sp"), lax.axis_size("tp")
    weight_list = (
        query_weight,
        forget_weight,
        value_matrix,
        output_gate_weight,
        after_gate_weight,
        before_gate_weight,
        convolution_input_weight,
    )
    query_raw, forget_raw, value_raw, outgate_raw, postgate_raw, pregate_raw, convval_raw = project(
        tp, layer_input, input_norm_gain[None, :], weight_list
    )
    partial_output, shifted_query, state_pieces, state_decays = local_pass(
        sp, query_raw, forget_raw, value_raw, surge_log_decay, forget_minimum[None, :]
    )
    return finish(
        sp,
        tp,
        partial_output,
        shifted_query,
        state_pieces,
        state_decays,
        starting_state,
        outgate_raw,
        postgate_raw,
        pregate_raw,
        convval_raw,
        convolution_kernel,
        head_norm_gain[None, :],
        recurrence_output_weight,
        convolution_output_weight,
        output_norm_gain[None, :],
    )


def solution(mesh):
    return jax.shard_map(
        shards,
        mesh=mesh,
        in_specs=(
            P("sp", "tp"),
            P(),
            P(None, "tp"),
            P(None, "tp"),
            P(None, "tp"),
            P(None, "tp"),
            P(None, "tp"),
            P(None, "tp"),
            P(None, "tp"),
            P("tp"),
            P("sp", "tp"),
            P(None, "tp"),
            P(),
            P("tp", "sp", None),
            P("tp", None),
            P("tp", None),
            P(),
        ),
        out_specs=P(("sp", "tp"), None),
        check_vma=False,
    )
```
